32 devices in a mesh: sp: 8 (over z, x), tp: 4 (over y, core).
Axes of the slice: x: 2, y: 2, z: 4, core: 2. Of those that a mesh axis runs over, the one named last changes fastest.
Arguments:
- query_one: bfloat16 [2048, 1024], P('sp', 'tp'), may hold values from -6 to 6
- key_one: bfloat16 [2048, 1024], P('sp', 'tp'), may hold values from -6 to 6
- value_one: bfloat16 [2048, 2048], P('sp', 'tp'), may hold values from -6 to 6
- gate_one: bfloat16 [2048, 2048], P('sp', 'tp'), may hold values from -6 to 6
- decay_one: float32 [2, 2048, 1024], P(None, 'sp', 'tp')
- query_two: bfloat16 [2048, 2048], P('sp', 'tp'), may hold values from -6 to 6
- key_two: bfloat16 [2048, 2048], P('sp', 'tp'), may hold values from -6 to 6
- value_two: bfloat16 [2048, 2048], P('sp', 'tp'), may hold values from -6 to 6
- gate_two: bfloat16 [2048, 2048], P('sp', 'tp'), may hold values from -6 to 6
- decay_two: float32 [2, 2048, 2048], P(None, 'sp', 'tp')
- head_gain: float32 [128], replicated, may hold values from 0.1 to 1.9
- proj_one: bfloat16 [2048, 2048], P('tp'), may hold values from -0.09375 to 0.09375
- proj_two: bfloat16 [2048, 2048], P('tp'), may hold values from -0.09375 to 0.09375
- stream: bfloat16 [2048, 2048], P('sp'), may hold values from -6 to 6
- gain_mix: float32 [2048], replicated, may hold values from 0.1 to 1.9
- gain_moe: float32 [2048], replicated, may hold values from 0.1 to 1.9
- routes: int32 [2048, 2], P('sp'), may hold values from 0 to 7, all different within a row; in each aligned block of 256 rows (0 to 255, 256 to 511, ...) at most 96 rows name the same one
- affinity: float32 [2048, 2], P('sp'), may hold values from 0.1 to 1
- expert_gate: bfloat16 [8, 2048, 2048], P('sp', None, 'tp'), may hold values from -0.125 to 0.125
- expert_up: bfloat16 [8, 2048, 2048], P('sp', None, 'tp'), may hold values from -0.125 to 0.125
- expert_down: bfloat16 [8, 2048, 2048], P('sp', 'tp'), may hold values from -0.125 to 0.125
Outputs:
- output: bfloat16 [2048, 2048], P(('sp', 'tp'))
The draws below stay inside these ranges and needn't reach their ends.
Inputs may be any that keep to these rules, and one draw needn't show every extreme that they name: `routes`: in the 256 rows of one index of sp no expert is named more than 96 times, a bound that some block reaches there in every draw; a row names 2 different experts.
All inputs are finite; a program needn't handle non-finite values.
Results may differ from the reference program's by a relative error of at most 0.017.
Values may be sent and summed in bfloat16 or wider, within the bound.
A program may use at most 64 MiB of HBM per device.

```python
import math
import jax
import jax.numpy as jnp
import numpy as np
from jax import lax

D = 2048
HEADS_A = 16
HEADS_B = 16
DK_A = 64
DK_B = 128
DV = 128
BLK = 64
FF_E = 2048
TOPK = 2
TOK_DEV = 256
STRING_LENGTH = 2048
EXPERTS = 8
CAP = 96
N_SP = 8
N_TP = 4


def decay_field(key, channels):
    keys = jax.random.split(key, 7)
    share = 0.5
    rapid_toggle = jax.random.bernoulli(keys[0], share, (2, 1, channels))
    quick = jax.random.uniform(keys[1], (2, 1, channels), jnp.float32, -0.5, 1.5)
    steady = math.log(STRING_LENGTH / 16.0) + jax.random.uniform(keys[2], (2, 1, channels), jnp.float32, 0.5, 1.5)
    floor_amount = jnp.where(rapid_toggle, quick, steady)
    spans = STRING_LENGTH // TOK_DEV
    additive_displacement = jnp.repeat(jax.random.uniform(keys[3], (2, spans, 1), jnp.float32, -0.7, 0.7), TOK_DEV, axis=1)
    jitter_magnitude = 0.7 * jax.random.truncated_normal(keys[4], -3.0, 3.0, (2, STRING_LENGTH, channels), jnp.float32)
    slot_numbers = jax.random.randint(keys[5], (2, 6), 0, STRING_LENGTH)
    sudden_jump = jnp.any(jnp.arange(STRING_LENGTH)[None, :, None] == slot_numbers[:, None, :], axis=2)[:, :, None]
    intensity_multiplier = jax.random.uniform(keys[6], (2, STRING_LENGTH, 1), jnp.float32, -11.0, -4.0)
    return jnp.where(sudden_jump & jnp.logical_not(rapid_toggle), intensity_multiplier, floor_amount + additive_displacement + jitter_magnitude).astype(jnp.float32)


def draw_decay_one(key, part):
    return decay_field(jax.random.fold_in(key, 11), HEADS_A * DK_A)


def draw_decay_two(key, part):
    return decay_field(jax.random.fold_in(key, 23), HEADS_B * DK_B)


def shard_levels(rng, shape, shards, smallest, high):
    level = 1.0
    for axis_at, shards_of in shards:
        heights = jax.random.uniform(jax.random.fold_in(jax.random.fold_in(rng, 6), axis_at), (shards_of,), jnp.float32, smallest / len(shards), high / len(shards))
        level = level * jnp.repeat(jnp.exp(heights), shape[axis_at] // shards_of).reshape((-1,) + (1,) * (len(shape) - 1 - axis_at))
    return level


def routed_block(stream_key, own, number, rows, count, top, bound, slope):
    ranking = jax.random.permutation(stream_key, count)
    packed, common = shares(count, rows * top, bound, slope, True), shares(count, rows * top, bound, slope, False)
    places = jnp.arange(count)

    def named(tallies, turn):
        used = int((tallies > 0).sum())
        fixed = max(1, used // 4)
        moved = fixed + (places - fixed + turn * (used - fixed)) % max(1, count - fixed)
        return jnp.zeros((count,), jnp.int32).at[ranking[jnp.where(places < fixed, places, moved)]].set(jnp.asarray(tallies, jnp.int32))

    tallies = jnp.where(number % 4 == 0, named(packed, number // 4), named(common, number - number // 4 - 1))
    mixed = jax.random.permutation(jax.random.fold_in(own, 3), count)
    donor, receiver = mixed[0:count // 2 * 2:2], mixed[1:count // 2 * 2:2]
    margin = jnp.minimum(tallies[donor] - 1, bound - tallies[receiver]) // 2
    margin = jnp.where((donor == ranking[0]) | (receiver == ranking[0]) | (tallies[receiver] == 0), 0, jnp.maximum(margin, 0))
    moved = jax.random.randint(jax.random.fold_in(own, 4), (count // 2,), 0, 1 << 20) % (margin + 1)
    tallies = tallies.at[donor].add(-moved).at[receiver].add(moved)
    labels = jnp.searchsorted(jnp.cumsum(tallies), jnp.arange(rows * top), side="right").astype(jnp.int32)
    listing = labels.reshape(top, rows).T
    listing = listing[jax.random.permutation(jax.random.fold_in(own, 1), rows)]
    turn = jax.random.randint(jax.random.fold_in(own, 2), (rows, 1), 0, top)
    return jnp.take_along_axis(listing, (jnp.arange(top)[None, :] + turn) % top, axis=1)


def shares(amount, total, bound, slope, full):
    loads = [(1 << 20) // math.isqrt(rank ** slope) + 1 for rank in range(1, amount + 1)]
    largest = bound if full else min(bound, max(-(-total // amount), total * loads[0] // sum(loads)))
    least = 1 if total - largest >= amount - 1 else 0
    given, rest = [largest] + [least] * (amount - 1), total - largest - least * (amount - 1)
    while rest > 0:
        movable = [i for i in range(1, amount) if given[i] < largest] or [i for i in range(1, amount) if given[i] < bound]
        pool, left = sum([loads[i] for i in movable]), rest
        for i in movable:
            addition = min(bound - given[i], max(1, left * loads[i] // pool), rest)
            given[i] = given[i] + addition
            rest = rest - addition
    return np.array(given)


def centred(own_key, extent, scale, limit, pieces=(), kind=jnp.bfloat16):
    values = jax.random.normal(own_key, extent, jnp.float32) * scale
    if len(pieces) > 0:
        values = shard_levels(own_key, extent, pieces, -0.22, 0.18) * values
    return jnp.clip(values, min=-limit, max=limit).astype(kind)


def setup_inputs(seed: int = 0) -> dict:
    seeds = jax.random.split(jax.random.key(seed), 22)
    query_one = centred(seeds[0], (STRING_LENGTH, HEADS_A * DK_A), 1.0, 6.0, ((0, 8), (1, 4)))
    key_one = centred(seeds[1], (STRING_LENGTH, HEADS_A * DK_A), 1.0, 6.0, ((0, 8), (1, 4)))
    value_one = centred(seeds[2], (STRING_LENGTH, HEADS_A * DV), 1.0, 6.0, ((0, 8), (1, 4)))
    gate_one = centred(seeds[3], (STRING_LENGTH, HEADS_A * DV), 1.0, 6.0, ((0, 8), (1, 4)))
    decay_one = draw_decay_one(jax.random.fold_in(seeds[21], 71), 0)
    query_two = centred(seeds[5], (STRING_LENGTH, HEADS_B * DK_B), 1.0, 6.0, ((0, 8), (1, 4)))
    key_two = centred(seeds[6], (STRING_LENGTH, HEADS_B * DK_B), 1.0, 6.0, ((0, 8), (1, 4)))
    value_two = centred(seeds[7], (STRING_LENGTH, HEADS_B * DV), 1.0, 6.0, ((0, 8), (1, 4)))
    gate_two = centred(seeds[8], (STRING_LENGTH, HEADS_B * DV), 1.0, 6.0, ((0, 8), (1, 4)))
    decay_two = draw_decay_two(jax.random.fold_in(seeds[21], 71), 0)
    head_gain = jnp.clip(1.0 + 0.18 * jax.random.normal(seeds[10], (DV,), jnp.float32), 0.1, 1.9)
    proj_one = centred(seeds[11], (HEADS_A * DV, D), ((HEADS_A + HEADS_B) * DV) ** -0.5, 0.09375, ((0, 4),))
    proj_two = centred(seeds[12], (HEADS_B * DV, D), ((HEADS_A + HEADS_B) * DV) ** -0.5, 0.09375, ((0, 4),))
    stream = centred(seeds[13], (STRING_LENGTH, D), 1.0, 6.0, ((0, 8),))
    gain_mix = jnp.clip(1.0 + 0.18 * jax.random.normal(seeds[14], (D,), jnp.float32), 0.1, 1.9)
    gain_moe = jnp.clip(1.0 + 0.18 * jax.random.normal(seeds[15], (D,), jnp.float32), 0.1, 1.9)
    routes_keys = jax.random.split(jax.random.fold_in(seeds[16], 1), STRING_LENGTH // TOK_DEV)
    routes_turns = jax.random.permutation(jax.random.fold_in(seeds[16], 3), STRING_LENGTH // TOK_DEV)
    routes = jax.vmap(lambda own, number: routed_block(jax.random.fold_in(seeds[16], 2), own, number, TOK_DEV, EXPERTS, TOPK, CAP, 2))(routes_keys, routes_turns).reshape((STRING_LENGTH, TOPK))
    affinity = jnp.clip(0.1 + 0.9 * jax.random.uniform(seeds[17], (STRING_LENGTH, TOPK), jnp.float32) ** shard_levels(seeds[17], (STRING_LENGTH, TOPK), ((0, 8),), -0.2, 0.2), 0.1, 1.0)
    expert_gate = centred(seeds[18], (EXPERTS, D, FF_E), D ** -0.5, 0.125, ((0, 8), (2, 4)))
    expert_up = centred(seeds[19], (EXPERTS, D, FF_E), D ** -0.5, 0.125, ((0, 8), (2, 4)))
    expert_down = centred(seeds[20], (EXPERTS, FF_E, D), FF_E ** -0.5, 0.125, ((0, 8), (1, 4)))
    return {"query_one": query_one, "key_one": key_one, "value_one": value_one, "gate_one": gate_one, "decay_one": decay_one, "query_two": query_two, "key_two": key_two, "value_two": value_two, "gate_two": gate_two, "decay_two": decay_two, "head_gain": head_gain, "proj_one": proj_one, "proj_two": proj_two, "stream": stream, "gain_mix": gain_mix, "gain_moe": gain_moe, "routes": routes, "affinity": affinity, "expert_gate": expert_gate, "expert_up": expert_up, "expert_down": expert_down}


normalizer_sharpness = 16.0
highest = lax.Precision.HIGHEST

def heads_first(values, heads):
    return values.reshape(values.shape[0], heads, -1).transpose(1, 0, 2)

def block_scan(query, key, value, logarithm_fading):
    heads, length, key_size = query.shape
    value_size = value.shape[-1]
    count = length // BLK

    def blocks(tensor):
        return tensor.reshape(heads, count, BLK, tensor.shape[-1])
    qb, kb, vb, gb = (blocks(query), blocks(key), blocks(value), blocks(logarithm_fading))
    cum = jnp.cumsum(gb, axis=2)
    last = cum[:, :, -1:, :]
    q_in = qb * jnp.exp(cum)
    k_in = kb * jnp.exp(-cum)
    k_st = kb * jnp.exp(last - cum)
    lower = jnp.tril(jnp.ones((BLK, BLK), dtype=bool))
    scores = jnp.where(lower, jnp.einsum('hnid,hnjd->hnij', q_in, k_in, precision=highest), 0.0)
    inner = jnp.einsum('hnij,hnjv->hniv', scores, vb, precision=highest)
    growth = jnp.einsum('hnjd,hnjv->hndv', k_st, vb, precision=highest)
    fading_speed = jnp.exp(last[:, :, 0, :])

    def step(state, inputs):
        factor, added = inputs
        return (factor[..., None] * state + added, state)
    final, starts = lax.scan(step, jnp.zeros((heads, key_size, value_size), jnp.float32), (fading_speed.transpose(1, 0, 2), growth.transpose(1, 0, 2, 3)))
    carried = jnp.einsum('hnid,hndv->hniv', q_in, starts.transpose(1, 0, 2, 3), precision=highest)
    return ((inner + carried).reshape(heads, length, value_size), final)

def group_mixed(query, key, value, fading_speed, key_size):
    heads = query.shape[1] // key_size
    qh = heads_first(query.astype(jnp.float32), heads) * key_size ** (-0.5)
    kh = heads_first(key.astype(jnp.float32), heads)
    vh = heads_first(value.astype(jnp.float32), heads)
    logarithm_fading = jax.nn.log_sigmoid(fading_speed) / normalizer_sharpness
    ahead = heads_first(logarithm_fading[0], heads)
    behind = heads_first(logarithm_fading[1], heads)
    forward, _ = block_scan(qh, kh, vh, ahead)
    backward, _ = block_scan(qh[:, ::-1], kh[:, ::-1], vh[:, ::-1], behind[:, ::-1])
    return forward + backward[:, ::-1]

def finish(mixed, gate, head_gain):
    normed = mixed * lax.rsqrt(lax.optimization_barrier(jnp.mean(mixed * mixed, axis=-1, keepdims=True)) + 1e-06) * head_gain
    flat = normed.transpose(1, 0, 2).reshape(mixed.shape[1], -1)
    return (flat * jax.nn.silu(gate.astype(jnp.float32))).astype(jnp.bfloat16)

def layer_norm(values, gain):
    mean = lax.optimization_barrier(jnp.mean(values, axis=-1, keepdims=True))
    spread = lax.optimization_barrier(jnp.mean(jnp.square(values - mean), axis=-1, keepdims=True))
    return (values - mean) * lax.rsqrt(spread + 1e-05) * gain

def reference(query_one, key_one, value_one, gate_one, decay_one, query_two, key_two, value_two, gate_two, decay_two, head_gain, proj_one, proj_two, stream, gain_mix, gain_moe, routes, affinity, expert_gate, expert_up, expert_down):
    heads_one = finish(group_mixed(query_one, key_one, value_one, decay_one, DK_A), gate_one, head_gain)
    heads_two = finish(group_mixed(query_two, key_two, value_two, decay_two, DK_B), gate_two, head_gain)
    width_one = HEADS_A // N_TP * DV
    width_two = HEADS_B // N_TP * DV
    total = jnp.zeros((STRING_LENGTH, D), jnp.float32)
    for block in range(N_TP):
        part = jnp.dot(heads_one[:, block * width_one:(block + 1) * width_one], proj_one[block * width_one:(block + 1) * width_one], preferred_element_type=jnp.float32)
        part = part + jnp.dot(heads_two[:, block * width_two:(block + 1) * width_two], proj_two[block * width_two:(block + 1) * width_two], preferred_element_type=jnp.float32)
        total = total + lax.optimization_barrier(part.astype(jnp.bfloat16)).astype(jnp.float32)
    attn = total.astype(jnp.bfloat16)
    settled = layer_norm(stream.astype(jnp.float32) + attn.astype(jnp.float32), gain_mix)
    moe_in = settled.astype(jnp.bfloat16)
    weights = (affinity / lax.optimization_barrier(jnp.sum(affinity, axis=-1, keepdims=True))).reshape(-1)
    assigned = STRING_LENGTH * TOPK
    flat_expert = routes.reshape(-1).astype(jnp.int32)
    order = jnp.argsort(flat_expert, stable=True).astype(jnp.int32)
    sorted_expert = flat_expert[order]
    counts = lax.optimization_barrier(jnp.sum((flat_expert[:, None] == jnp.arange(EXPERTS, dtype=jnp.int32)[None, :]).astype(jnp.int32), axis=0)).astype(jnp.int32)
    starts = (jnp.cumsum(counts).astype(jnp.int32) - counts).astype(jnp.int32)
    most_rows = N_SP * CAP
    slot = (jnp.arange(assigned, dtype=jnp.int32) - starts[sorted_expert]).astype(jnp.int32)
    table = jnp.full((EXPERTS * most_rows,), -1, jnp.int32).at[sorted_expert * most_rows + slot].set(order)
    table = table.reshape(EXPERTS, most_rows)
    unit_block = FF_E // N_TP

    def per_expert(acc, expert):
        entries = table[expert]
        valid = entries >= 0
        safe = jnp.where(valid, entries, 0).astype(jnp.int32)
        token = (safe // TOPK).astype(jnp.int32)
        rows = moe_in[token]
        gate = jnp.dot(rows, expert_gate[expert], preferred_element_type=jnp.float32)
        upward = jnp.dot(rows, expert_up[expert], preferred_element_type=jnp.float32)
        act = (jax.nn.silu(gate) * upward).astype(jnp.bfloat16)
        act_blocks = act.astype(jnp.float32).reshape(most_rows, N_TP, unit_block)
        down_blocks = expert_down[expert].astype(jnp.float32).reshape(N_TP, unit_block, D)
        partial_value = jnp.einsum('rbf,bfd->rbd', act_blocks, down_blocks, precision=highest)
        rounded = lax.optimization_barrier(partial_value.astype(jnp.bfloat16)).astype(jnp.float32)
        piece = lax.optimization_barrier(lax.optimization_barrier(jnp.sum(rounded, axis=1)).astype(jnp.bfloat16)).astype(jnp.float32)
        scale = jnp.where(valid, weights[safe], 0.0)
        return (acc.at[token].add(scale[:, None] * piece), None)
    mixture, _ = lax.scan(per_expert, jnp.zeros((STRING_LENGTH, D), jnp.float32), jnp.arange(EXPERTS, dtype=jnp.int32))
    return layer_norm(settled + mixture, gain_moe).astype(jnp.bfloat16)
```

```python
import functools

import jax
import jax.numpy as jnp
from jax import lax
from jax.experimental import pallas as pl
from jax.experimental.pallas import tpu as pltpu
from jax.sharding import PartitionSpec as P

DK_A = 64
DK_B = 128
BLK = 64
SHARPNESS = 16.0
F32 = jnp.float32
BF16 = jnp.bfloat16
MESH = pl.DeviceIdType.MESH
VMEM = pl.BlockSpec(memory_space=pltpu.VMEM)
DMA = pltpu.SemaphoreType.DMA


def params(collective_id=None):
    if collective_id is None:
        return pltpu.CompilerParams(vmem_limit_bytes=48 * 2**20)
    return pltpu.CompilerParams(
        vmem_limit_bytes=48 * 2**20, collective_id=collective_id, has_side_effects=True
    )


def mm(a, b):
    return jnp.dot(a, b, preferred_element_type=F32)


def mm_nt(a, b):
    return lax.dot_general(a, b, (((1,), (1,)), ((), ())), preferred_element_type=F32)


def mm_tn(a, b):
    return lax.dot_general(a, b, (((0,), (0,)), ((), ())), preferred_element_type=F32)


def log_sigmoid(x):
    return jnp.minimum(x, 0.0) - jnp.log1p(jnp.exp(-jnp.abs(x)))


def silu(x):
    return x / (1.0 + jnp.exp(-x))


def layer_norm(values, gain):
    mean = jnp.mean(values, axis=-1, keepdims=True)
    spread = jnp.mean(jnp.square(values - mean), axis=-1, keepdims=True)
    return (values - mean) * lax.rsqrt(spread + 1e-05) * gain


def greet(peers):
    barrier = pltpu.get_barrier_semaphore()
    for peer in peers:
        pl.semaphore_signal(barrier, inc=1, device_id=peer, device_id_type=MESH)
    pl.semaphore_wait(barrier, len(peers))


def remote(src, dst, send, recv, peer):
    return pltpu.make_async_remote_copy(
        src_ref=src, dst_ref=dst, send_sem=send, recv_sem=recv, device_id=peer, device_id_type=MESH
    )


def state_kernel(ka, va, da, kb, vb, db, stack, cum):
    rows = ka.shape[0]
    count = rows // BLK
    ii = lax.broadcasted_iota(jnp.int32, (rows, rows), 0)
    jj = lax.broadcasted_iota(jnp.int32, (rows, rows), 1)
    same = (ii // BLK) == (jj // BLK)
    lower = jnp.where(same & (ii >= jj), 1.0, 0.0).astype(BF16)
    upper = jnp.where(same & (ii <= jj), 1.0, 0.0).astype(BF16)
    base = 0
    for k, v, d, dk in ((ka, va, da, DK_A), (kb, vb, db, DK_B)):
        wide = k.shape[1]
        heads = wide // dk
        dv = v.shape[1] // heads
        keys = k[...].astype(F32)
        for way in range(2):
            fade = log_sigmoid(d[way]) / SHARPNESS
            high = fade.astype(BF16)
            low = (fade - high.astype(F32)).astype(BF16)
            tri = lower if way == 0 else upper
            total = mm(tri, high) + mm(tri, low)
            cum[way, :, base : base + wide] = total
            tail = jnp.zeros((1, wide), F32)
            weighted = [None] * count
            for b in reversed(range(count)) if way == 0 else range(count):
                part = total[b * BLK : (b + 1) * BLK]
                last = part[BLK - 1 : BLK] if way == 0 else part[0:1]
                weighted[b] = (keys[b * BLK : (b + 1) * BLK] * jnp.exp(last - part + tail)).astype(BF16)
                tail = tail + last
            weighted = jnp.concatenate(weighted, axis=0)
            states = [
                mm_tn(v[:, h * dv : (h + 1) * dv], weighted[:, h * dk : (h + 1) * dk]).astype(BF16)
                for h in range(heads)
            ]
            stack[way, 0:dv, base : base + wide] = (
                states[0] if heads == 1 else jnp.concatenate(states, axis=1)
            )
            thigh = tail.astype(BF16).astype(F32)
            row = lax.broadcasted_iota(jnp.int32, (16, wide), 0)
            stack[way, dv : dv + 16, base : base + wide] = jnp.where(
                row == 0, thigh, jnp.where(row == 1, tail - thigh, 0.0)
            ).astype(BF16)
        base += wide


def states_exchange_kernel(n, x, out, send, recv):
    me = lax.axis_index("sp")
    greet([{"sp": lax.rem(me + k, n)} for k in range(1, n)])
    copies = []
    for k in range(1, n):
        peer = lax.rem(me + k, n)
        way = jnp.where(peer < me, 1, 0)
        copy = remote(x.at[way], out.at[me], send.at[k], recv.at[k], {"sp": peer})
        copy.start()
        copies.append(copy)
    for k in range(1, n):
        peer = lax.rem(me + k, n)
        copies[k - 1].wait_send()
        remote(x.at[0], out.at[lax.rem(me + n - k, n)], send.at[k], recv.at[k], {"sp": peer}).wait_recv()


def mix_kernel(
    n, states, cum, qa, ka, va, ga, qb, kb, vb, gb, gain, pa, pb, out, heads_ref, ahead, behind
):
    me = lax.axis_index("sp")
    rows = qa.shape[0]
    count = rows // BLK
    dv = ahead.shape[0]
    ahead[...] = jnp.zeros_like(ahead)
    behind[...] = jnp.zeros_like(behind)

    def join(total, source):
        fade = states[source, dv : dv + 1, :].astype(F32) + states[source, dv + 1 : dv + 2, :].astype(F32)
        total[...] = jnp.exp(fade) * total[...] + states[source, 0:dv, :].astype(F32)

    def one(s, carry):
        @pl.when(s < me)
        def _():
            join(ahead, s)

        back = n - 1 - s

        @pl.when(back > me)
        def _():
            join(behind, back)

        return carry

    lax.fori_loop(0, n, one, 0)
    ii = lax.broadcasted_iota(jnp.int32, (BLK, BLK), 0)
    jj = lax.broadcasted_iota(jnp.int32, (BLK, BLK), 1)
    base = 0
    column = 0
    for q, k, v, g, dk in ((qa, ka, va, ga, DK_A), (qb, kb, vb, gb, DK_B)):
        heads = q.shape[1] // dk
        for h in range(heads):
            lanes = slice(base + h * dk, base + (h + 1) * dk)
            own = slice(h * dk, (h + 1) * dk)
            vown = slice(h * dv, (h + 1) * dv)
            forward = ahead[:, lanes]
            backward = behind[:, lanes]
            mixed = [None] * count
            readers = [None] * count
            growth = [None] * count
            for b in range(count):
                at = slice(b * BLK, (b + 1) * BLK)
                query = q[at, own].astype(F32) * dk ** (-0.5)
                key = k[at, own].astype(F32)
                value = v[at, vown]
                cf = cum[0, at, lanes]
                cb = cum[1, at, lanes]
                qf = (query * jnp.exp(cf)).astype(BF16)
                kf = (key * jnp.exp(-cf)).astype(BF16)
                qr = (query * jnp.exp(cb)).astype(BF16)
                kr = (key * jnp.exp(-cb)).astype(BF16)
                scores = jnp.where(ii >= jj, mm_nt(qf, kf), 0.0) + jnp.where(ii <= jj, mm_nt(qr, kr), 0.0)
                inner = mm(scores.astype(BF16), value)
                lastf = cf[BLK - 1 : BLK]
                inner = inner + mm_nt(qf, forward.astype(BF16))
                if b < count - 1:
                    kfs = (key * jnp.exp(lastf - cf)).astype(BF16)
                    forward = jnp.exp(lastf) * forward + mm_tn(value, kfs)
                mixed[b] = inner
                readers[b] = qr
                lastb = cb[0:1]
                if b > 0:
                    kbs = (key * jnp.exp(lastb - cb)).astype(BF16)
                    growth[b] = (jnp.exp(lastb), mm_tn(value, kbs))
            for b in reversed(range(count)):
                at = slice(b * BLK, (b + 1) * BLK)
                whole = mixed[b] + mm_nt(readers[b], backward.astype(BF16))
                if b > 0:
                    backward = growth[b][0] * backward + growth[b][1]
                scale = lax.rsqrt(jnp.mean(whole * whole, axis=-1, keepdims=True) + 1e-06)
                heads_ref[at, column + h * dv : column + (h + 1) * dv] = (
                    whole * scale * gain[...] * silu(g[at, vown].astype(F32))
                ).astype(BF16)
        base += heads * dk
        column += heads * dv
    split = pa.shape[0]
    width = out.shape[1]
    tile = min(512, width)
    for j in range(width // tile):
        cols = slice(j * tile, (j + 1) * tile)
        out[:, cols] = (
            mm(heads_ref[:, :split], pa[:, cols]) + mm(heads_ref[:, split:], pb[:, cols])
        ).astype(BF16)


def settle_kernel(n, part, stream, gain, settled, columns, inbox, outbox, send, recv, send2, recv2):
    me = lax.axis_index("tp")
    own = part.shape[0] // n
    wide = part.shape[1] // n
    greet([{"tp": lax.rem(me + k, n)} for k in range(1, n)])

    def rows_of(i):
        return pl.ds(pl.multiple_of(i * own, own), own)

    def cols_of(i):
        return pl.ds(pl.multiple_of(i * wide, wide), wide)

    copies = []
    for k in range(1, n):
        peer = lax.rem(me + k, n)
        copy = remote(part.at[rows_of(peer), :], inbox.at[k], send.at[k], recv.at[k], {"tp": peer})
        copy.start()
        copies.append(copy)
    total = part[rows_of(me), :].astype(F32)
    for k in range(1, n):
        copies[k - 1].wait_recv()
        total = total + inbox[k].astype(F32)
    total = total.astype(BF16).astype(F32)
    value = layer_norm(stream[rows_of(me), :].astype(F32) + total, gain[...])
    settled[...] = value
    outbox[...] = value.astype(BF16)
    second = []
    for k in range(1, n):
        peer = lax.rem(me + k, n)
        copy = remote(
            outbox.at[:, cols_of(peer)], columns.at[rows_of(me), :], send2.at[k], recv2.at[k], {"tp": peer}
        )
        copy.start()
        second.append(copy)
    columns[rows_of(me), :] = outbox[:, cols_of(me)]
    for k in range(1, n):
        source = lax.rem(me + n - k, n)
        copies[k - 1].wait_send()
        second[k - 1].wait_send()
        remote(
            outbox.at[:, cols_of(source)], columns.at[rows_of(source), :], send2.at[k], recv2.at[k], {"tp": source}
        ).wait_recv()


def slots_of(routes, capacity, experts):
    rows, top = routes.shape
    lane = lax.broadcasted_iota(jnp.int32, (rows, max(128, experts)), 1)
    hots = [routes[:, i : i + 1] == lane for i in range(top)]
    named = sum(jnp.where(h, 1.0, 0.0) for h in hots)
    ii = lax.broadcasted_iota(jnp.int32, (rows, rows), 0)
    jj = lax.broadcasted_iota(jnp.int32, (rows, rows), 1)
    before = mm(jnp.where(ii > jj, 1.0, 0.0).astype(BF16), named.astype(BF16))
    slots = []
    for i in range(top):
        rank = jnp.sum(jnp.where(hots[i], before, 0.0), axis=1, keepdims=True).astype(jnp.int32)
        slots.append(routes[:, i : i + 1] * capacity + rank)
    return slots


def pick_kernel(capacity, experts, routes, columns, out):
    slots = slots_of(routes[...], capacity, experts)
    rows = columns.shape[0]
    lane = lax.broadcasted_iota(jnp.int32, (rows, experts * capacity), 1)
    hot = sum(jnp.where(lane == s, 1.0, 0.0) for s in slots).astype(BF16)
    out[...] = mm_tn(hot, columns[...]).astype(BF16)


def dispatch_kernel(n, m, x, out, ss, sr, ys, yr, cs, cr, fs, fr, local):
    me = lax.axis_index("sp")
    my = lax.axis_index("tp")
    wide = x.shape[2]
    core = lax.rem(my, 2)
    line = my // 2
    lines = m // 2
    partner = my + 1 - 2 * core

    def cols_of(i):
        return pl.ds(pl.multiple_of(i * wide, wide), wide)

    def line_peer(j):
        return lax.rem(line + j, lines) * 2 + core

    def line_source(j):
        return lax.rem(line + lines - j, lines) * 2 + core

    greet(
        [{"sp": lax.rem(me + k, n)} for k in range(1, n)]
        + [{"tp": partner}]
        + [{"tp": line_peer(j)} for j in range(1, lines)]
    )

    def cross(k):
        peer = lax.rem(me + k, n)
        return remote(x.at[peer], out.at[me, :, cols_of(my)], ss.at[k], sr.at[k], {"sp": peer})

    for k in range(1, n):
        cross(k).start()
    own = pltpu.make_async_copy(x.at[me], out.at[me, :, cols_of(my)], local)
    own.start()

    def block(s, i):
        return out.at[s, :, cols_of(i)]

    def to_line(k, s, j, i):
        return remote(block(s, i), block(s, i), ys.at[k, j], yr.at[k, j], {"tp": line_peer(j)})

    def to_core(k, s, i):
        return remote(block(s, i), block(s, i), cs.at[k], cr.at[k], {"tp": partner})

    def forward(k, s, j, i):
        return remote(block(s, i), block(s, i), fs.at[k, j], fr.at[k, j], {"tp": partner})

    def source(k):
        return lax.rem(me + n - k, n)

    def hand_on(k, s):
        for j in range(1, lines):
            to_line(k, s, j, my).start()
        to_core(k, s, my).start()

    def pass_on(k, s):
        for j in range(1, lines):
            i = line_source(j)
            to_line(k, s, j, i).wait_recv()
            forward(k, s, j, i).start()

    own.wait()
    hand_on(0, me)
    for k in range(1, n):
        s = source(k)
        remote(x.at[0], block(s, my), ss.at[k], sr.at[k], {"sp": s}).wait_recv()
        hand_on(k, s)
        pass_on(k - 1, source(k - 1))
    pass_on(n - 1, source(n - 1))
    for k in range(n):
        s = source(k)
        if k > 0:
            cross(k).wait_send()
        to_core(k, s, my).wait_send()
        to_core(k, s, partner).wait_recv()
        for j in range(1, lines):
            i = line_source(j)
            to_line(k, s, j, my).wait_send()
            forward(k, s, j, i).wait_send()
            forward(k, s, j, i + 1 - 2 * core).wait_recv()


def return_kernel(n, m, x, out, inbox, mid, midbox, last, cs, cr, ys, yr, ss, sr):
    me = lax.axis_index("sp")
    my = lax.axis_index("tp")
    wide = out.shape[2]
    core = lax.rem(my, 2)
    line = my // 2
    lines = m // 2
    partner = my + 1 - 2 * core

    def cols_of(i):
        return pl.ds(pl.multiple_of(i * wide, wide), wide)

    def line_at(j):
        return lax.rem(line + j, lines)

    greet(
        [{"sp": lax.rem(me + k, n)} for k in range(1, n)]
        + [{"tp": partner}]
        + [{"tp": line_at(j) * 2 + core} for j in range(1, lines)]
    )

    def place(k):
        return lax.rem(me + k + 1, n)

    def to_core(k, j):
        i = line_at(j) * 2 + 1 - core
        return remote(x.at[place(k), :, cols_of(i)], inbox.at[k, j], cs.at[k, j], cr.at[k, j], {"tp": partner})

    def to_line(k, j):
        return remote(
            mid.at[k, j], midbox.at[k, j], ys.at[k, j], yr.at[k, j], {"tp": line_at(j) * 2 + core}
        )

    def cross(k):
        peer = place(k)
        return remote(last.at[k], out.at[me], ss.at[k], sr.at[k], {"sp": peer})

    for k in range(n):
        for j in reversed(range(lines)):
            to_core(k, j).start()

    def first(k):
        for j in reversed(range(lines)):
            to_core(k, j).wait_recv()
            i = line_at(j) * 2 + core
            mine = x[place(k), :, cols_of(i)].astype(F32) + inbox[k, j].astype(F32)
            mid[k, j] = mine.astype(BF16)
            if j > 0:
                to_line(k, j).start()

    def second(k):
        total = mid[k, 0].astype(F32)
        for j in range(1, lines):
            to_line(k, j).wait_recv()
            total = total + midbox[k, j].astype(F32)
        if k < n - 1:
            last[k] = total.astype(BF16)
            cross(k).start()
        else:
            out[me] = total.astype(BF16)

    first(0)
    for k in range(1, n):
        first(k)
        second(k - 1)
    second(n - 1)
    for k in range(n):
        for j in range(lines):
            to_core(k, j).wait_send()
            if j > 0:
                to_line(k, j).wait_send()
        if k < n - 1:
            cross(k).wait_send()
            s = lax.rem(me + 2 * n - k - 1, n)
            remote(last.at[k], out.at[s], ss.at[k], sr.at[k], {"sp": s}).wait_recv()


def finish_kernel(n, capacity, experts, routes, affinity, pieces, settled, gain, out, term, mixture, send, recv):
    me = lax.axis_index("tp")
    rows = routes.shape[0]
    own = rows // n
    wide = pieces.shape[1]
    greet([{"tp": lax.rem(me + k, n)} for k in range(1, n)])

    def rows_of(i):
        return pl.ds(pl.multiple_of(i * own, own), own)

    def cols_of(i):
        return pl.ds(pl.multiple_of(i * wide, wide), wide)

    slots = slots_of(routes[...], capacity, experts)
    weights = affinity[...] / jnp.sum(affinity[...], axis=-1, keepdims=True)
    lane = lax.broadcasted_iota(jnp.int32, (rows, experts * capacity), 1)
    total = jnp.zeros((rows, wide), F32)
    for i, slot in enumerate(slots):
        hot = jnp.where(lane == slot, 1.0, 0.0).astype(BF16)
        total = total + weights[:, i : i + 1] * mm(hot, pieces[...])
    term[...] = total.astype(BF16)
    copies = []
    for k in range(1, n):
        peer = lax.rem(me + k, n)
        copy = remote(term.at[rows_of(peer), :], mixture.at[:, cols_of(me)], send.at[k], recv.at[k], {"tp": peer})
        copy.start()
        copies.append(copy)
    mixture[:, cols_of(me)] = term[rows_of(me), :]
    for k in range(1, n):
        source = lax.rem(me + n - k, n)
        copies[k - 1].wait_send()
        remote(
            term.at[rows_of(source), :], mixture.at[:, cols_of(source)], send.at[k], recv.at[k], {"tp": source}
        ).wait_recv()
    out[...] = layer_norm(settled[...] + mixture[...].astype(F32), gain[...]).astype(BF16)


def call(kernel, outs, scratch, count, collective_id=None):
    single = not isinstance(outs, list)
    return pl.pallas_call(
        kernel,
        out_shape=outs,
        in_specs=[VMEM] * count,
        out_specs=VMEM if single else [VMEM] * len(outs),
        scratch_shapes=scratch,
        compiler_params=params(collective_id),
    )


def body(
    query_one,
    key_one,
    value_one,
    gate_one,
    decay_one,
    query_two,
    key_two,
    value_two,
    gate_two,
    decay_two,
    head_gain,
    proj_one,
    proj_two,
    stream,
    gain_mix,
    gain_moe,
    routes,
    affinity,
    expert_gate,
    expert_up,
    expert_down,
):
    shape = jax.ShapeDtypeStruct
    rows = query_one.shape[0]
    n = lax.axis_size("sp")
    m = lax.axis_size("tp")
    width = stream.shape[1]
    own = rows // m
    wide = width // m
    dv = head_gain.shape[0]
    lanes = query_one.shape[1] + query_two.shape[1]
    values = value_one.shape[1] + value_two.shape[1]
    local_experts = expert_gate.shape[0]
    experts = local_experts * n
    top = routes.shape[1]
    capacity = 3 * rows * top // (2 * experts)
    room = local_experts * capacity

    stack, cum = call(
        state_kernel, [shape((2, dv + 16, lanes), BF16), shape((2, rows, lanes), F32)], [], 6
    )(key_one, value_one, decay_one, key_two, value_two, decay_two)
    states = call(
        functools.partial(states_exchange_kernel, n),
        shape((n, dv + 16, lanes), BF16),
        [DMA((n,)), DMA((n,))],
        1,
        1,
    )(stack)
    part = call(
        functools.partial(mix_kernel, n),
        shape((rows, width), BF16),
        [pltpu.VMEM((rows, values), BF16), pltpu.VMEM((dv, lanes), F32), pltpu.VMEM((dv, lanes), F32)],
        13,
    )(
        states, cum, query_one, key_one, value_one, gate_one, query_two, key_two, value_two, gate_two,
        head_gain.reshape(1, -1), proj_one, proj_two,
    )
    settled, columns = call(
        functools.partial(settle_kernel, m),
        [shape((own, width), F32), shape((rows, wide), BF16)],
        [pltpu.VMEM((m, own, width), BF16), pltpu.VMEM((own, width), BF16)] + [DMA((m,))] * 4,
        3,
        2,
    )(part, stream, gain_mix.reshape(1, -1))
    outgoing = call(
        functools.partial(pick_kernel, capacity, experts), shape((experts * capacity, wide), BF16), [], 2
    )(routes, columns)
    lines = m // 2
    received = call(
        functools.partial(dispatch_kernel, n, m),
        shape((n, room, width), BF16),
        [DMA((n,)), DMA((n,)), DMA((n, lines)), DMA((n, lines)), DMA((n,)), DMA((n,)),
         DMA((n, lines)), DMA((n, lines)), DMA],
        1,
        3,
    )(outgoing.reshape(n, room, wide))
    x = received.reshape(n, local_experts, capacity, width)
    results = []
    for e in range(local_experts):
        xe = x[:, e].reshape(n * capacity, width)
        gate = mm(xe, expert_gate[e])
        upward = mm(xe, expert_up[e])
        act = (jax.nn.silu(gate) * upward).astype(BF16)
        results.append(mm(act, expert_down[e]).astype(BF16).reshape(n, capacity, width))
    partial_value = results[0] if local_experts == 1 else jnp.concatenate(results, axis=1)
    pieces = call(
        functools.partial(return_kernel, n, m),
        shape((n, room, wide), BF16),
        [pltpu.VMEM((n, lines, room, wide), BF16)] * 3
        + [pltpu.VMEM((n, room, wide), BF16)]
        + [DMA((n, lines))] * 4
        + [DMA((n,))] * 2,
        1,
        4,
    )(partial_value)
    return call(
        functools.partial(finish_kernel, m, capacity, experts),
        shape((own, width), BF16),
        [pltpu.VMEM((rows, wide), BF16), pltpu.VMEM((own, width), BF16), DMA((m,)), DMA((m,))],
        5,
        5,
    )(routes, affinity, pieces.reshape(experts * capacity, wide), settled, gain_moe.reshape(1, -1))


def solution(mesh):
    return jax.shard_map(
        body,
        mesh=mesh,
        in_specs=(
            P("sp", "tp"),
            P("sp", "tp"),
            P("sp", "tp"),
            P("sp", "tp"),
            P(None, "sp", "tp"),
            P("sp", "tp"),
            P("sp", "tp"),
            P("sp", "tp"),
            P("sp", "tp"),
            P(None, "sp", "tp"),
            P(),
            P("tp", None),
            P("tp", None),
            P("sp", None),
            P(),
            P(),
            P("sp", None),
            P("sp", None),
            P("sp", None, "tp"),
            P("sp", None, "tp"),
            P("sp", "tp", None),
        ),
        out_specs=P(("sp", "tp"), None),
        check_vma=False,
    )
```

```python
import functools

import jax
import jax.numpy as jnp
from jax import lax
from jax.experimental import pallas as pl
from jax.experimental.pallas import tpu as pltpu
from jax.sharding import PartitionSpec as P

DK_A = 64
DK_B = 128
BLK = 64
SHARPNESS = 16.0
F32 = jnp.float32
BF16 = jnp.bfloat16
MESH = pl.DeviceIdType.MESH
VMEM = pl.BlockSpec(memory_space=pltpu.VMEM)
DMA = pltpu.SemaphoreType.DMA


def params(collective_id=None):
    if collective_id is None:
        return pltpu.CompilerParams(vmem_limit_bytes=48 * 2**20)
    return pltpu.CompilerParams(
        vmem_limit_bytes=48 * 2**20, collective_id=collective_id, has_side_effects=True
    )


def mm(a, b):
    return jnp.dot(a, b, preferred_element_type=F32)


def mm_nt(a, b):
    return lax.dot_general(a, b, (((1,), (1,)), ((), ())), preferred_element_type=F32)


def mm_tn(a, b):
    return lax.dot_general(a, b, (((0,), (0,)), ((), ())), preferred_element_type=F32)


def log_sigmoid(x):
    return jnp.minimum(x, 0.0) - jnp.log1p(jnp.exp(-jnp.abs(x)))


def silu(x):
    return x / (1.0 + jnp.exp(-x))


def layer_norm(values, gain):
    mean = jnp.mean(values, axis=-1, keepdims=True)
    spread = jnp.mean(jnp.square(values - mean), axis=-1, keepdims=True)
    return (values - mean) * lax.rsqrt(spread + 1e-05) * gain


def greet(peers):
    barrier = pltpu.get_barrier_semaphore()
    for peer in peers:
        pl.semaphore_signal(barrier, inc=1, device_id=peer, device_id_type=MESH)
    pl.semaphore_wait(barrier, len(peers))


def remote(src, dst, send, recv, peer):
    return pltpu.make_async_remote_copy(
        src_ref=src, dst_ref=dst, send_sem=send, recv_sem=recv, device_id=peer, device_id_type=MESH
    )


def across(me, k, n):
    place, bit = 0, 1
    while bit < n:
        digit = lax.rem(me // bit, 2)
        place = place + (1 - digit if k & bit else digit) * bit
        bit *= 2
    return place


def state_kernel(ka, va, da, kb, vb, db, stack, cum):
    rows = ka.shape[0]
    count = rows // BLK
    ii = lax.broadcasted_iota(jnp.int32, (rows, rows), 0)
    jj = lax.broadcasted_iota(jnp.int32, (rows, rows), 1)
    same = (ii // BLK) == (jj // BLK)
    lower = jnp.where(same & (ii >= jj), 1.0, 0.0).astype(BF16)
    upper = jnp.where(same & (ii <= jj), 1.0, 0.0).astype(BF16)
    base = 0
    for k, v, d, dk in ((ka, va, da, DK_A), (kb, vb, db, DK_B)):
        wide = k.shape[1]
        heads = wide // dk
        dv = v.shape[1] // heads
        keys = k[...].astype(F32)
        for way in range(2):
            fade = log_sigmoid(d[way]) / SHARPNESS
            high = fade.astype(BF16)
            low = (fade - high.astype(F32)).astype(BF16)
            tri = lower if way == 0 else upper
            total = mm(tri, high) + mm(tri, low)
            cum[way, :, base : base + wide] = total
            tail = jnp.zeros((1, wide), F32)
            weighted = [None] * count
            for b in reversed(range(count)) if way == 0 else range(count):
                part = total[b * BLK : (b + 1) * BLK]
                last = part[BLK - 1 : BLK] if way == 0 else part[0:1]
                weighted[b] = (keys[b * BLK : (b + 1) * BLK] * jnp.exp(last - part + tail)).astype(BF16)
                tail = tail + last
            weighted = jnp.concatenate(weighted, axis=0)
            states = [
                mm_tn(v[:, h * dv : (h + 1) * dv], weighted[:, h * dk : (h + 1) * dk]).astype(BF16)
                for h in range(heads)
            ]
            states = states[0] if heads == 1 else jnp.concatenate(states, axis=1)
            thigh = tail.astype(BF16).astype(F32)
            row = lax.broadcasted_iota(jnp.int32, (16, wide), 0)
            fades = jnp.where(row == 0, thigh, jnp.where(row == 1, tail - thigh, 0.0)).astype(BF16)
            half = dv // 2
            for i in range(2):
                stack[i, way, 0:half, base : base + wide] = states[i * half : (i + 1) * half]
                stack[i, way, half : half + 16, base : base + wide] = fades
        base += wide


def spread(total, wide):
    row = lax.broadcasted_iota(jnp.int32, (16, wide), 0)
    high = total.astype(BF16).astype(F32)
    return jnp.where(row == 0, high, jnp.where(row == 1, total - high, 0.0)).astype(BF16)


def states_exchange_kernel(n, stack, out, xbox, agg, zbox, outbox, xs, xr, zs, zr, bs, br):
    me = lax.axis_index("sp")
    side = lax.rem(me, 2)
    pair = me // 2
    pairs = n // 2
    partner = me + 1 - 2 * side
    half = out.shape[2]
    lanes = out.shape[3]
    chunk = 256 if lanes % 256 == 0 else lanes
    count = lanes // chunk

    def pair_at(j):
        return lax.rem(pair + j, pairs)

    greet([{"sp": partner}] + [{"sp": pair_at(j) * 2 + side} for j in range(1, pairs)])

    def at(c):
        return pl.ds(c * chunk, chunk)

    def swap(c):
        return remote(
            stack.at[1 - side, :, :, at(c)], xbox.at[:, :, at(c)], xs.at[c], xr.at[c], {"sp": partner}
        )

    def along(c, j):
        way = jnp.where(pair_at(j) < pair, 1, 0)
        return remote(
            agg.at[way, :, at(c)], zbox.at[pair, :, at(c)], zs.at[c, j], zr.at[c, j],
            {"sp": pair_at(j) * 2 + side},
        )

    def back(c):
        return remote(
            outbox.at[:, :, at(c)], out.at[:, side, :, at(c)], bs.at[c], br.at[c], {"sp": partner}
        )

    for c in range(count):
        swap(c).start()
    zbox[pair] = jnp.zeros_like(zbox[pair])

    def load(ref, index, c):
        block = ref[index + (slice(None), at(c))].astype(F32)
        return block[0:half], block[half : half + 1] + block[half + 1 : half + 2]

    def both(c, way):
        own, own_fade = load(stack, (side, way), c)
        other, other_fade = load(xbox, (way,), c)
        low = side == 0
        return (
            jnp.where(low, own, other), jnp.where(low, own_fade, other_fade),
            jnp.where(low, other, own), jnp.where(low, other_fade, own_fade),
        )

    for c in range(count):
        swap(c).wait_recv()
        s0, t0, s1, t1 = both(c, 0)
        agg[0, 0:half, at(c)] = (jnp.exp(t1) * s0 + s1).astype(BF16)
        agg[0, half : half + 16, at(c)] = spread(t0 + t1, chunk)
        s0, t0, s1, t1 = both(c, 1)
        agg[1, 0:half, at(c)] = (jnp.exp(t0) * s1 + s0).astype(BF16)
        agg[1, half : half + 16, at(c)] = spread(t0 + t1, chunk)
        for j in range(1, pairs):
            along(c, j).start()
    for c in range(count):
        for j in range(1, pairs):
            along(c, j).wait_recv()
        ahead = jnp.zeros((half, chunk), F32)
        behind = jnp.zeros((half, chunk), F32)
        for s in range(pairs):
            state, fade = load(zbox, (s,), c)
            ahead = jnp.where(s < pair, jnp.exp(fade) * ahead + state, ahead)
        for s in reversed(range(pairs)):
            state, fade = load(zbox, (s,), c)
            behind = jnp.where(s > pair, jnp.exp(fade) * behind + state, behind)
        low = side == 0
        s0, t0, _, _ = both(c, 0)
        next_ahead = jnp.exp(t0) * ahead + s0
        _, _, s1, t1 = both(c, 1)
        next_behind = jnp.exp(t1) * behind + s1
        outbox[0, :, at(c)] = jnp.where(low, next_ahead, ahead).astype(BF16)
        outbox[1, :, at(c)] = jnp.where(low, behind, next_behind).astype(BF16)
        back(c).start()
        out[0, side, :, at(c)] = jnp.where(low, ahead, next_ahead).astype(BF16)
        out[1, side, :, at(c)] = jnp.where(low, next_behind, behind).astype(BF16)
    for c in range(count):
        swap(c).wait_send()
        for j in range(1, pairs):
            along(c, j).wait_send()
        back(c).wait_send()
        remote(
            outbox.at[:, :, at(c)], out.at[:, 1 - side, :, at(c)], bs.at[c], br.at[c], {"sp": partner}
        ).wait_recv()


def mix_kernel(states, cum, qa, ka, va, ga, qb, kb, vb, gb, gain, pa, pb, out, heads_ref):
    rows = qa.shape[0]
    count = rows // BLK
    dv = gain.shape[1]
    ii = lax.broadcasted_iota(jnp.int32, (BLK, BLK), 0)
    jj = lax.broadcasted_iota(jnp.int32, (BLK, BLK), 1)
    base = 0
    column = 0
    for q, k, v, g, dk in ((qa, ka, va, ga, DK_A), (qb, kb, vb, gb, DK_B)):
        heads = q.shape[1] // dk
        for h in range(heads):
            lanes = slice(base + h * dk, base + (h + 1) * dk)
            own = slice(h * dk, (h + 1) * dk)
            vown = slice(h * dv, (h + 1) * dv)
            forward = jnp.concatenate([states[0, i, :, lanes] for i in range(2)], axis=0).astype(F32)
            backward = jnp.concatenate([states[1, i, :, lanes] for i in range(2)], axis=0).astype(F32)
            mixed = [None] * count
            readers = [None] * count
            growth = [None] * count
            for b in range(count):
                at = slice(b * BLK, (b + 1) * BLK)
                query = q[at, own].astype(F32) * dk ** (-0.5)
                key = k[at, own].astype(F32)
                value = v[at, vown]
                cf = cum[0, at, lanes]
                cb = cum[1, at, lanes]
                qf = (query * jnp.exp(cf)).astype(BF16)
                kf = (key * jnp.exp(-cf)).astype(BF16)
                qr = (query * jnp.exp(cb)).astype(BF16)
                kr = (key * jnp.exp(-cb)).astype(BF16)
                scores = jnp.where(ii >= jj, mm_nt(qf, kf), 0.0) + jnp.where(ii <= jj, mm_nt(qr, kr), 0.0)
                inner = mm(scores.astype(BF16), value)
                lastf = cf[BLK - 1 : BLK]
                inner = inner + mm_nt(qf, forward.astype(BF16))
                if b < count - 1:
                    kfs = (key * jnp.exp(lastf - cf)).astype(BF16)
                    forward = jnp.exp(lastf) * forward + mm_tn(value, kfs)
                mixed[b] = inner
                readers[b] = qr
                lastb = cb[0:1]
                if b > 0:
                    kbs = (key * jnp.exp(lastb - cb)).astype(BF16)
                    growth[b] = (jnp.exp(lastb), mm_tn(value, kbs))
            for b in reversed(range(count)):
                at = slice(b * BLK, (b + 1) * BLK)
                whole = mixed[b] + mm_nt(readers[b], backward.astype(BF16))
                if b > 0:
                    backward = growth[b][0] * backward + growth[b][1]
                scale = lax.rsqrt(jnp.mean(whole * whole, axis=-1, keepdims=True) + 1e-06)
                heads_ref[at, column + h * dv : column + (h + 1) * dv] = (
                    whole * scale * gain[...] * silu(g[at, vown].astype(F32))
                ).astype(BF16)
        base += heads * dk
        column += heads * dv
    split = pa.shape[0]
    width = out.shape[1]
    tile = min(512, width)
    for j in range(width // tile):
        cols = slice(j * tile, (j + 1) * tile)
        out[:, cols] = (
            mm(heads_ref[:, :split], pa[:, cols]) + mm(heads_ref[:, split:], pb[:, cols])
        ).astype(BF16)


def settle_kernel(
    n, part, stream, gain, settled, columns, inbox, mid, midbox, outbox, cs, cr, ys, yr, send2, recv2
):
    me = lax.axis_index("tp")
    own = part.shape[0] // n
    wide = part.shape[1] // n
    core = lax.rem(me, 2)
    line = me // 2
    lines = n // 2
    greet([{"tp": lax.rem(me + k, n)} for k in range(1, n)])

    def rows_of(i):
        return pl.ds(pl.multiple_of(i * own, own), own)

    def cols_of(i):
        return pl.ds(pl.multiple_of(i * wide, wide), wide)

    def line_at(j):
        return lax.rem(line + j, lines)

    def to_core(j):
        i = line_at(j) * 2 + 1 - core
        return remote(
            part.at[rows_of(i), :], inbox.at[j], cs.at[j], cr.at[j], {"tp": me + 1 - 2 * core}
        )

    def to_line(j):
        return remote(mid.at[j], midbox.at[j], ys.at[j], yr.at[j], {"tp": line_at(j) * 2 + core})

    for j in reversed(range(lines)):
        to_core(j).start()
    for j in reversed(range(lines)):
        to_core(j).wait_recv()
        mine = part[rows_of(line_at(j) * 2 + core), :].astype(F32) + inbox[j].astype(F32)
        if j > 0:
            mid[j] = mine.astype(BF16)
            to_line(j).start()
        else:
            total = mine
    for j in range(1, lines):
        to_line(j).wait_recv()
        total = total + midbox[j].astype(F32)
    total = total.astype(BF16).astype(F32)
    value = layer_norm(stream[rows_of(me), :].astype(F32) + total, gain[...])
    settled[...] = value
    outbox[...] = value.astype(BF16)
    second = []
    for k in range(1, n):
        peer = lax.rem(me + k, n)
        copy = remote(
            outbox.at[:, cols_of(peer)], columns.at[rows_of(me), :], send2.at[k], recv2.at[k], {"tp": peer}
        )
        copy.start()
        second.append(copy)
    columns[rows_of(me), :] = outbox[:, cols_of(me)]
    for k in range(1, n):
        source = lax.rem(me + n - k, n)
        second[k - 1].wait_send()
        remote(
            outbox.at[:, cols_of(source)], columns.at[rows_of(source), :], send2.at[k], recv2.at[k], {"tp": source}
        ).wait_recv()
    for j in range(lines):
        to_core(j).wait_send()
        if j > 0:
            to_line(j).wait_send()


def slots_of(routes, capacity, experts):
    rows, top = routes.shape
    lane = lax.broadcasted_iota(jnp.int32, (rows, max(128, experts)), 1)
    hots = [routes[:, i : i + 1] == lane for i in range(top)]
    named = sum(jnp.where(h, 1.0, 0.0) for h in hots)
    ii = lax.broadcasted_iota(jnp.int32, (rows, rows), 0)
    jj = lax.broadcasted_iota(jnp.int32, (rows, rows), 1)
    before = mm(jnp.where(ii > jj, 1.0, 0.0).astype(BF16), named.astype(BF16))
    slots = []
    for i in range(top):
        rank = jnp.sum(jnp.where(hots[i], before, 0.0), axis=1, keepdims=True).astype(jnp.int32)
        slots.append(routes[:, i : i + 1] * capacity + rank)
    return slots


def pick_kernel(capacity, experts, routes, columns, out):
    slots = slots_of(routes[...], capacity, experts)
    rows = columns.shape[0]
    lane = lax.broadcasted_iota(jnp.int32, (rows, experts * capacity), 1)
    hot = sum(jnp.where(lane == s, 1.0, 0.0) for s in slots).astype(BF16)
    out[...] = mm_tn(hot, columns[...]).astype(BF16)


def dispatch_kernel(n, m, x, out, ss, sr, ys, yr, cs, cr, fs, fr, local):
    me = lax.axis_index("sp")
    my = lax.axis_index("tp")
    wide = x.shape[2]
    core = lax.rem(my, 2)
    line = my // 2
    lines = m // 2
    partner = my + 1 - 2 * core

    def cols_of(i):
        return pl.ds(pl.multiple_of(i * wide, wide), wide)

    def line_peer(j):
        return lax.rem(line + j, lines) * 2 + core

    def line_source(j):
        return lax.rem(line + lines - j, lines) * 2 + core

    greet(
        [{"sp": lax.rem(me + k, n)} for k in range(1, n)]
        + [{"tp": partner}]
        + [{"tp": line_peer(j)} for j in range(1, lines)]
    )

    def cross(k):
        peer = across(me, k, n)
        return remote(x.at[peer], out.at[me, :, cols_of(my)], ss.at[k], sr.at[k], {"sp": peer})

    for k in range(1, n):
        cross(k).start()
    own = pltpu.make_async_copy(x.at[me], out.at[me, :, cols_of(my)], local)
    own.start()

    def block(s, i):
        return out.at[s, :, cols_of(i)]

    def to_line(k, s, j, i):
        return remote(block(s, i), block(s, i), ys.at[k, j], yr.at[k, j], {"tp": line_peer(j)})

    def to_core(k, s, i):
        return remote(block(s, i), block(s, i), cs.at[k], cr.at[k], {"tp": partner})

    def forward(k, s, j, i):
        return remote(block(s, i), block(s, i), fs.at[k, j], fr.at[k, j], {"tp": partner})

    def source(k):
        return across(me, k, n)

    def hand_on(k, s):
        for j in range(1, lines):
            to_line(k, s, j, my).start()
        to_core(k, s, my).start()

    def pass_on(k, s):
        for j in range(1, lines):
            i = line_source(j)
            to_line(k, s, j, i).wait_recv()
            forward(k, s, j, i).start()

    own.wait()
    hand_on(0, me)
    for k in range(1, n):
        s = source(k)
        remote(x.at[0], block(s, my), ss.at[k], sr.at[k], {"sp": s}).wait_recv()
        hand_on(k, s)
        pass_on(k - 1, source(k - 1))
    pass_on(n - 1, source(n - 1))
    for k in range(n):
        s = source(k)
        if k > 0:
            cross(k).wait_send()
        to_core(k, s, my).wait_send()
        to_core(k, s, partner).wait_recv()
        for j in range(1, lines):
            i = line_source(j)
            to_line(k, s, j, my).wait_send()
            forward(k, s, j, i).wait_send()
            forward(k, s, j, i + 1 - 2 * core).wait_recv()


def return_kernel(n, m, x, out, inbox, mid, midbox, last, cs, cr, ys, yr, ss, sr):
    me = lax.axis_index("sp")
    my = lax.axis_index("tp")
    wide = out.shape[2]
    core = lax.rem(my, 2)
    line = my // 2
    lines = m // 2
    partner = my + 1 - 2 * core

    def cols_of(i):
        return pl.ds(pl.multiple_of(i * wide, wide), wide)

    def line_at(j):
        return lax.rem(line + j, lines)

    greet(
        [{"sp": lax.rem(me + k, n)} for k in range(1, n)]
        + [{"tp": partner}]
        + [{"tp": line_at(j) * 2 + core} for j in range(1, lines)]
    )

    def place(k):
        return across(me, n - 1 - k, n)

    def to_core(k, j):
        i = line_at(j) * 2 + 1 - core
        return remote(x.at[place(k), :, cols_of(i)], inbox.at[k, j], cs.at[k, j], cr.at[k, j], {"tp": partner})

    def to_line(k, j):
        return remote(
            mid.at[k, j], midbox.at[k, j], ys.at[k, j], yr.at[k, j], {"tp": line_at(j) * 2 + core}
        )

    def cross(k):
        peer = place(k)
        return remote(last.at[k], out.at[me], ss.at[k], sr.at[k], {"sp": peer})

    for k in range(n):
        for j in reversed(range(lines)):
            to_core(k, j).start()

    def first(k):
        for j in reversed(range(lines)):
            to_core(k, j).wait_recv()
            i = line_at(j) * 2 + core
            mine = x[place(k), :, cols_of(i)].astype(F32) + inbox[k, j].astype(F32)
            mid[k, j] = mine.astype(BF16)
            if j > 0:
                to_line(k, j).start()

    def second(k):
        total = mid[k, 0].astype(F32)
        for j in range(1, lines):
            to_line(k, j).wait_recv()
            total = total + midbox[k, j].astype(F32)
        if k < n - 1:
            last[k] = total.astype(BF16)
            cross(k).start()
        else:
            out[me] = total.astype(BF16)

    first(0)
    for k in range(1, n):
        first(k)
        second(k - 1)
    second(n - 1)
    for k in range(n):
        for j in range(lines):
            to_core(k, j).wait_send()
            if j > 0:
                to_line(k, j).wait_send()
        if k < n - 1:
            cross(k).wait_send()
            s = place(k)
            remote(last.at[k], out.at[s], ss.at[k], sr.at[k], {"sp": s}).wait_recv()


def finish_kernel(n, capacity, experts, routes, affinity, pieces, settled, gain, out, term, mixture, send, recv):
    me = lax.axis_index("tp")
    rows = routes.shape[0]
    own = rows // n
    wide = pieces.shape[1]
    greet([{"tp": lax.rem(me + k, n)} for k in range(1, n)])

    def rows_of(i):
        return pl.ds(pl.multiple_of(i * own, own), own)

    def cols_of(i):
        return pl.ds(pl.multiple_of(i * wide, wide), wide)

    slots = slots_of(routes[...], capacity, experts)
    weights = affinity[...] / jnp.sum(affinity[...], axis=-1, keepdims=True)
    lane = lax.broadcasted_iota(jnp.int32, (rows, experts * capacity), 1)
    total = jnp.zeros((rows, wide), F32)
    for i, slot in enumerate(slots):
        hot = jnp.where(lane == slot, 1.0, 0.0).astype(BF16)
        total = total + weights[:, i : i + 1] * mm(hot, pieces[...])
    term[...] = total.astype(BF16)
    copies = []
    for k in range(1, n):
        peer = lax.rem(me + k, n)
        copy = remote(term.at[rows_of(peer), :], mixture.at[:, cols_of(me)], send.at[k], recv.at[k], {"tp": peer})
        copy.start()
        copies.append(copy)
    mixture[:, cols_of(me)] = term[rows_of(me), :]
    for k in range(1, n):
        source = lax.rem(me + n - k, n)
        copies[k - 1].wait_send()
        remote(
            term.at[rows_of(source), :], mixture.at[:, cols_of(source)], send.at[k], recv.at[k], {"tp": source}
        ).wait_recv()
    out[...] = layer_norm(settled[...] + mixture[...].astype(F32), gain[...]).astype(BF16)


def call(kernel, outs, scratch, count, collective_id=None):
    single = not isinstance(outs, list)
    return pl.pallas_call(
        kernel,
        out_shape=outs,
        in_specs=[VMEM] * count,
        out_specs=VMEM if single else [VMEM] * len(outs),
        scratch_shapes=scratch,
        compiler_params=params(collective_id),
    )


def body(
    query_one,
    key_one,
    value_one,
    gate_one,
    decay_one,
    query_two,
    key_two,
    value_two,
    gate_two,
    decay_two,
    head_gain,
    proj_one,
    proj_two,
    stream,
    gain_mix,
    gain_moe,
    routes,
    affinity,
    expert_gate,
    expert_up,
    expert_down,
):
    shape = jax.ShapeDtypeStruct
    rows = query_one.shape[0]
    n = lax.axis_size("sp")
    m = lax.axis_size("tp")
    width = stream.shape[1]
    own = rows // m
    wide = width // m
    dv = head_gain.shape[0]
    lanes = query_one.shape[1] + query_two.shape[1]
    values = value_one.shape[1] + value_two.shape[1]
    local_experts = expert_gate.shape[0]
    experts = local_experts * n
    top = routes.shape[1]
    capacity = 3 * rows * top // (2 * experts)
    room = local_experts * capacity

    half = dv // 2
    stack, cum = call(
        state_kernel, [shape((2, 2, half + 16, lanes), BF16), shape((2, rows, lanes), F32)], [], 6
    )(key_one, value_one, decay_one, key_two, value_two, decay_two)
    chunks = max(1, lanes // 256)
    states = call(
        functools.partial(states_exchange_kernel, n),
        shape((2, 2, half, lanes), BF16),
        [
            pltpu.VMEM((2, half + 16, lanes), BF16),
            pltpu.VMEM((2, half + 16, lanes), BF16),
            pltpu.VMEM((n // 2, half + 16, lanes), BF16),
            pltpu.VMEM((2, half, lanes), BF16),
            DMA((chunks,)), DMA((chunks,)), DMA((chunks, n // 2)), DMA((chunks, n // 2)),
            DMA((chunks,)), DMA((chunks,)),
        ],
        1,
        1,
    )(stack)
    part = call(mix_kernel, shape((rows, width), BF16), [pltpu.VMEM((rows, values), BF16)], 13)(
        states, cum, query_one, key_one, value_one, gate_one, query_two, key_two, value_two, gate_two,
        head_gain.reshape(1, -1), proj_one, proj_two,
    )
    settled, columns = call(
        functools.partial(settle_kernel, m),
        [shape((own, width), F32), shape((rows, wide), BF16)],
        [pltpu.VMEM((m // 2, own, width), BF16)] * 3
        + [pltpu.VMEM((own, width), BF16)]
        + [DMA((m // 2,))] * 4
        + [DMA((m,))] * 2,
        3,
        2,
    )(part, stream, gain_mix.reshape(1, -1))
    outgoing = call(
        functools.partial(pick_kernel, capacity, experts), shape((experts * capacity, wide), BF16), [], 2
    )(routes, columns)
    lines = m // 2
    received = call(
        functools.partial(dispatch_kernel, n, m),
        shape((n, room, width), BF16),
        [DMA((n,)), DMA((n,)), DMA((n, lines)), DMA((n, lines)), DMA((n,)), DMA((n,)),
         DMA((n, lines)), DMA((n, lines)), DMA],
        1,
        3,
    )(outgoing.reshape(n, room, wide))
    x = received.reshape(n, local_experts, capacity, width)
    results = []
    for e in range(local_experts):
        xe = x[:, e].reshape(n * capacity, width)
        gate = mm(xe, expert_gate[e])
        upward = mm(xe, expert_up[e])
        act = (jax.nn.silu(gate) * upward).astype(BF16)
        results.append(mm(act, expert_down[e]).astype(BF16).reshape(n, capacity, width))
    partial_value = results[0] if local_experts == 1 else jnp.concatenate(results, axis=1)
    pieces = call(
        functools.partial(return_kernel, n, m),
        shape((n, room, wide), BF16),
        [pltpu.VMEM((n, lines, room, wide), BF16)] * 3
        + [pltpu.VMEM((n, room, wide), BF16)]
        + [DMA((n, lines))] * 4
        + [DMA((n,))] * 2,
        1,
        4,
    )(partial_value)
    return call(
        functools.partial(finish_kernel, m, capacity, experts),
        shape((own, width), BF16),
        [pltpu.VMEM((rows, wide), BF16), pltpu.VMEM((own, width), BF16), DMA((m,)), DMA((m,))],
        5,
        5,
    )(routes, affinity, pieces.reshape(experts * capacity, wide), settled, gain_moe.reshape(1, -1))


def solution(mesh):
    return jax.shard_map(
        body,
        mesh=mesh,
        in_specs=(
            P("sp", "tp"),
            P("sp", "tp"),
            P("sp", "tp"),
            P("sp", "tp"),
            P(None, "sp", "tp"),
            P("sp", "tp"),
            P("sp", "tp"),
            P("sp", "tp"),
            P("sp", "tp"),
            P(None, "sp", "tp"),
            P(),
            P("tp", None),
            P("tp", None),
            P("sp", None),
            P(),
            P(),
            P("sp", None),
            P("sp", None),
            P("sp", None, "tp"),
            P("sp", None, "tp"),
            P("sp", "tp", None),
        ),
        out_specs=P(("sp", "tp"), None),
        check_vma=False,
    )
```

```python
import functools

import jax
import jax.numpy as jnp
from jax import lax
from jax.experimental import pallas as pl
from jax.experimental.pallas import tpu as pltpu
from jax.sharding import PartitionSpec as P

DK_A = 64
DK_B = 128
BLK = 64
SHARPNESS = 16.0
F32 = jnp.float32
BF16 = jnp.bfloat16
MESH = pl.DeviceIdType.MESH
VMEM = pl.BlockSpec(memory_space=pltpu.VMEM)
DMA = pltpu.SemaphoreType.DMA


def params(collective_id=None):
    if collective_id is None:
        return pltpu.CompilerParams(vmem_limit_bytes=48 * 2**20)
    return pltpu.CompilerParams(
        vmem_limit_bytes=48 * 2**20, collective_id=collective_id, has_side_effects=True
    )


def mm(a, b):
    return jnp.dot(a, b, preferred_element_type=F32)


def mm_nt(a, b):
    return lax.dot_general(a, b, (((1,), (1,)), ((), ())), preferred_element_type=F32)


def mm_tn(a, b):
    return lax.dot_general(a, b, (((0,), (0,)), ((), ())), preferred_element_type=F32)


def log_sigmoid(x):
    return jnp.minimum(x, 0.0) - jnp.log1p(jnp.exp(-jnp.abs(x)))


def silu(x):
    return x / (1.0 + jnp.exp(-x))


def layer_norm(values, gain):
    mean = jnp.mean(values, axis=-1, keepdims=True)
    spread = jnp.mean(jnp.square(values - mean), axis=-1, keepdims=True)
    return (values - mean) * lax.rsqrt(spread + 1e-05) * gain


def greet(peers):
    barrier = pltpu.get_barrier_semaphore()
    for peer in peers:
        pl.semaphore_signal(barrier, inc=1, device_id=peer, device_id_type=MESH)
    pl.semaphore_wait(barrier, len(peers))


def remote(src, dst, send, recv, peer):
    return pltpu.make_async_remote_copy(
        src_ref=src, dst_ref=dst, send_sem=send, recv_sem=recv, device_id=peer, device_id_type=MESH
    )


def across(me, k, n):
    place, bit = 0, 1
    while bit < n:
        digit = lax.rem(me // bit, 2)
        place = place + (1 - digit if k & bit else digit) * bit
        bit *= 2
    return place


def state_kernel(*refs):
    held, stack, cum, local, sems = refs[:6], refs[6], refs[7], refs[8:14], refs[14]
    loads = [pltpu.make_async_copy(a, b, sems.at[i]) for i, (a, b) in enumerate(zip(held, local))]
    for load in loads:
        load.start()
    for load in loads:
        load.wait()
    ka, va, da, kb, vb, db = local
    rows = ka.shape[0]
    count = rows // BLK
    ii = lax.broadcasted_iota(jnp.int32, (rows, rows), 0)
    jj = lax.broadcasted_iota(jnp.int32, (rows, rows), 1)
    same = (ii // BLK) == (jj // BLK)
    lower = jnp.where(same & (ii >= jj), 1.0, 0.0).astype(BF16)
    upper = jnp.where(same & (ii <= jj), 1.0, 0.0).astype(BF16)
    base = 0
    for k, v, d, dk in ((ka, va, da, DK_A), (kb, vb, db, DK_B)):
        wide = k.shape[1]
        heads = wide // dk
        dv = v.shape[1] // heads
        keys = k[...].astype(F32)
        for way in range(2):
            fade = log_sigmoid(d[way]) / SHARPNESS
            high = fade.astype(BF16)
            low = (fade - high.astype(F32)).astype(BF16)
            tri = lower if way == 0 else upper
            total = mm(tri, high) + mm(tri, low)
            cum[way, :, base : base + wide] = total
            tail = jnp.zeros((1, wide), F32)
            weighted = [None] * count
            for b in reversed(range(count)) if way == 0 else range(count):
                part = total[b * BLK : (b + 1) * BLK]
                last = part[BLK - 1 : BLK] if way == 0 else part[0:1]
                weighted[b] = (keys[b * BLK : (b + 1) * BLK] * jnp.exp(last - part + tail)).astype(BF16)
                tail = tail + last
            weighted = jnp.concatenate(weighted, axis=0)
            states = [
                mm_tn(v[:, h * dv : (h + 1) * dv], weighted[:, h * dk : (h + 1) * dk]).astype(BF16)
                for h in range(heads)
            ]
            states = states[0] if heads == 1 else jnp.concatenate(states, axis=1)
            thigh = tail.astype(BF16).astype(F32)
            row = lax.broadcasted_iota(jnp.int32, (16, wide), 0)
            fades = jnp.where(row == 0, thigh, jnp.where(row == 1, tail - thigh, 0.0)).astype(BF16)
            half = dv // 2
            for i in range(2):
                stack[i, way, 0:half, base : base + wide] = states[i * half : (i + 1) * half]
                stack[i, way, half : half + 16, base : base + wide] = fades
        base += wide


def spread(total, wide):
    row = lax.broadcasted_iota(jnp.int32, (16, wide), 0)
    high = total.astype(BF16).astype(F32)
    return jnp.where(row == 0, high, jnp.where(row == 1, total - high, 0.0)).astype(BF16)


def states_exchange_kernel(n, stack, out, xbox, agg, zbox, outbox, xs, xr, zs, zr, bs, br):
    me = lax.axis_index("sp")
    side = lax.rem(me, 2)
    pair = me // 2
    pairs = n // 2
    partner = me + 1 - 2 * side
    half = out.shape[2]
    lanes = out.shape[3]
    chunk = 256 if lanes % 256 == 0 else lanes
    count = lanes // chunk

    def pair_at(j):
        return lax.rem(pair + j, pairs)

    greet([{"sp": partner}] + [{"sp": pair_at(j) * 2 + side} for j in range(1, pairs)])

    def at(c):
        return pl.ds(c * chunk, chunk)

    def swap(c):
        return remote(
            stack.at[1 - side, :, :, at(c)], xbox.at[:, :, at(c)], xs.at[c], xr.at[c], {"sp": partner}
        )

    def along(c, j):
        way = jnp.where(pair_at(j) < pair, 1, 0)
        return remote(
            agg.at[way, :, at(c)], zbox.at[pair, :, at(c)], zs.at[c, j], zr.at[c, j],
            {"sp": pair_at(j) * 2 + side},
        )

    def back(c):
        return remote(
            outbox.at[:, :, at(c)], out.at[:, side, :, at(c)], bs.at[c], br.at[c], {"sp": partner}
        )

    for c in range(count):
        swap(c).start()
    zbox[pair] = jnp.zeros_like(zbox[pair])

    def load(ref, index, c):
        block = ref[index + (slice(None), at(c))].astype(F32)
        return block[0:half], block[half : half + 1] + block[half + 1 : half + 2]

    def both(c, way):
        own, own_fade = load(stack, (side, way), c)
        other, other_fade = load(xbox, (way,), c)
        low = side == 0
        return (
            jnp.where(low, own, other), jnp.where(low, own_fade, other_fade),
            jnp.where(low, other, own), jnp.where(low, other_fade, own_fade),
        )

    for c in range(count):
        swap(c).wait_recv()
        s0, t0, s1, t1 = both(c, 0)
        agg[0, 0:half, at(c)] = (jnp.exp(t1) * s0 + s1).astype(BF16)
        agg[0, half : half + 16, at(c)] = spread(t0 + t1, chunk)
        s0, t0, s1, t1 = both(c, 1)
        agg[1, 0:half, at(c)] = (jnp.exp(t0) * s1 + s0).astype(BF16)
        agg[1, half : half + 16, at(c)] = spread(t0 + t1, chunk)
        for j in range(1, pairs):
            along(c, j).start()
    for c in range(count):
        for j in range(1, pairs):
            along(c, j).wait_recv()
        ahead = jnp.zeros((half, chunk), F32)
        behind = jnp.zeros((half, chunk), F32)
        for s in range(pairs):
            state, fade = load(zbox, (s,), c)
            ahead = jnp.where(s < pair, jnp.exp(fade) * ahead + state, ahead)
        for s in reversed(range(pairs)):
            state, fade = load(zbox, (s,), c)
            behind = jnp.where(s > pair, jnp.exp(fade) * behind + state, behind)
        low = side == 0
        s0, t0, _, _ = both(c, 0)
        next_ahead = jnp.exp(t0) * ahead + s0
        _, _, s1, t1 = both(c, 1)
        next_behind = jnp.exp(t1) * behind + s1
        outbox[0, :, at(c)] = jnp.where(low, next_ahead, ahead).astype(BF16)
        outbox[1, :, at(c)] = jnp.where(low, behind, next_behind).astype(BF16)
        back(c).start()
        out[0, side, :, at(c)] = jnp.where(low, ahead, next_ahead).astype(BF16)
        out[1, side, :, at(c)] = jnp.where(low, next_behind, behind).astype(BF16)
    for c in range(count):
        swap(c).wait_send()
        for j in range(1, pairs):
            along(c, j).wait_send()
        back(c).wait_send()
        remote(
            outbox.at[:, :, at(c)], out.at[:, 1 - side, :, at(c)], bs.at[c], br.at[c], {"sp": partner}
        ).wait_recv()


def mix_kernel(states, cum, qa, ka, va, ga, qb, kb, vb, gb, gain, pa, pb, out, heads_ref):
    rows = qa.shape[0]
    count = rows // BLK
    dv = gain.shape[1]
    ii = lax.broadcasted_iota(jnp.int32, (BLK, BLK), 0)
    jj = lax.broadcasted_iota(jnp.int32, (BLK, BLK), 1)
    base = 0
    column = 0
    for q, k, v, g, dk in ((qa, ka, va, ga, DK_A), (qb, kb, vb, gb, DK_B)):
        heads = q.shape[1] // dk
        for h in range(heads):
            lanes = slice(base + h * dk, base + (h + 1) * dk)
            own = slice(h * dk, (h + 1) * dk)
            vown = slice(h * dv, (h + 1) * dv)
            forward = jnp.concatenate([states[0, i, :, lanes] for i in range(2)], axis=0).astype(F32)
            backward = jnp.concatenate([states[1, i, :, lanes] for i in range(2)], axis=0).astype(F32)
            mixed = [None] * count
            readers = [None] * count
            growth = [None] * count
            for b in range(count):
                at = slice(b * BLK, (b + 1) * BLK)
                query = q[at, own].astype(F32) * dk ** (-0.5)
                key = k[at, own].astype(F32)
                value = v[at, vown]
                cf = cum[0, at, lanes]
                cb = cum[1, at, lanes]
                qf = (query * jnp.exp(cf)).astype(BF16)
                kf = (key * jnp.exp(-cf)).astype(BF16)
                qr = (query * jnp.exp(cb)).astype(BF16)
                kr = (key * jnp.exp(-cb)).astype(BF16)
                scores = jnp.where(ii >= jj, mm_nt(qf, kf), 0.0) + jnp.where(ii <= jj, mm_nt(qr, kr), 0.0)
                inner = mm(scores.astype(BF16), value)
                lastf = cf[BLK - 1 : BLK]
                inner = inner + mm_nt(qf, forward.astype(BF16))
                if b < count - 1:
                    kfs = (key * jnp.exp(lastf - cf)).astype(BF16)
                    forward = jnp.exp(lastf) * forward + mm_tn(value, kfs)
                mixed[b] = inner
                readers[b] = qr
                lastb = cb[0:1]
                if b > 0:
                    kbs = (key * jnp.exp(lastb - cb)).astype(BF16)
                    growth[b] = (jnp.exp(lastb), mm_tn(value, kbs))
            for b in reversed(range(count)):
                at = slice(b * BLK, (b + 1) * BLK)
                whole = mixed[b] + mm_nt(readers[b], backward.astype(BF16))
                if b > 0:
                    backward = growth[b][0] * backward + growth[b][1]
                scale = lax.rsqrt(jnp.mean(whole * whole, axis=-1, keepdims=True) + 1e-06)
                heads_ref[at, column + h * dv : column + (h + 1) * dv] = (
                    whole * scale * gain[...] * silu(g[at, vown].astype(F32))
                ).astype(BF16)
        base += heads * dk
        column += heads * dv
    split = pa.shape[0]
    width = out.shape[1]
    tile = min(512, width)
    for j in range(width // tile):
        cols = slice(j * tile, (j + 1) * tile)
        out[:, cols] = (
            mm(heads_ref[:, :split], pa[:, cols]) + mm(heads_ref[:, split:], pb[:, cols])
        ).astype(BF16)


def settle_kernel(
    n, part, stream, gain, settled, columns, inbox, mid, midbox, outbox, cs, cr, ys, yr, send2, recv2
):
    me = lax.axis_index("tp")
    own = part.shape[0] // n
    wide = part.shape[1] // n
    core = lax.rem(me, 2)
    line = me // 2
    lines = n // 2
    greet([{"tp": lax.rem(me + k, n)} for k in range(1, n)])

    def rows_of(i):
        return pl.ds(pl.multiple_of(i * own, own), own)

    def cols_of(i):
        return pl.ds(pl.multiple_of(i * wide, wide), wide)

    def line_at(j):
        return lax.rem(line + j, lines)

    def to_core(j):
        i = line_at(j) * 2 + 1 - core
        return remote(
            part.at[rows_of(i), :], inbox.at[j], cs.at[j], cr.at[j], {"tp": me + 1 - 2 * core}
        )

    def to_line(j):
        return remote(mid.at[j], midbox.at[j], ys.at[j], yr.at[j], {"tp": line_at(j) * 2 + core})

    for j in reversed(range(lines)):
        to_core(j).start()
    for j in reversed(range(lines)):
        to_core(j).wait_recv()
        mine = part[rows_of(line_at(j) * 2 + core), :].astype(F32) + inbox[j].astype(F32)
        if j > 0:
            mid[j] = mine.astype(BF16)
            to_line(j).start()
        else:
            total = mine
    for j in range(1, lines):
        to_line(j).wait_recv()
        total = total + midbox[j].astype(F32)
    total = total.astype(BF16).astype(F32)
    value = layer_norm(stream[rows_of(me), :].astype(F32) + total, gain[...])
    settled[...] = value
    outbox[...] = value.astype(BF16)
    second = []
    for k in range(1, n):
        peer = lax.rem(me + k, n)
        copy = remote(
            outbox.at[:, cols_of(peer)], columns.at[rows_of(me), :], send2.at[k], recv2.at[k], {"tp": peer}
        )
        copy.start()
        second.append(copy)
    columns[rows_of(me), :] = outbox[:, cols_of(me)]
    for k in range(1, n):
        source = lax.rem(me + n - k, n)
        second[k - 1].wait_send()
        remote(
            outbox.at[:, cols_of(source)], columns.at[rows_of(source), :], send2.at[k], recv2.at[k], {"tp": source}
        ).wait_recv()
    for j in range(lines):
        to_core(j).wait_send()
        if j > 0:
            to_line(j).wait_send()


def slots_of(routes, capacity, experts):
    rows, top = routes.shape
    lane = lax.broadcasted_iota(jnp.int32, (rows, max(128, experts)), 1)
    hots = [routes[:, i : i + 1] == lane for i in range(top)]
    named = sum(jnp.where(h, 1.0, 0.0) for h in hots)
    ii = lax.broadcasted_iota(jnp.int32, (rows, rows), 0)
    jj = lax.broadcasted_iota(jnp.int32, (rows, rows), 1)
    before = mm(jnp.where(ii > jj, 1.0, 0.0).astype(BF16), named.astype(BF16))
    slots = []
    for i in range(top):
        rank = jnp.sum(jnp.where(hots[i], before, 0.0), axis=1, keepdims=True).astype(jnp.int32)
        slots.append(routes[:, i : i + 1] * capacity + rank)
    return slots


def pick_kernel(capacity, experts, routes, columns, out):
    slots = slots_of(routes[...], capacity, experts)
    rows = columns.shape[0]
    lane = lax.broadcasted_iota(jnp.int32, (rows, experts * capacity), 1)
    hot = sum(jnp.where(lane == s, 1.0, 0.0) for s in slots).astype(BF16)
    out[...] = mm_tn(hot, columns[...]).astype(BF16)


def dispatch_kernel(n, m, x, out, ss, sr, ys, yr, cs, cr, fs, fr, local):
    me = lax.axis_index("sp")
    my = lax.axis_index("tp")
    wide = x.shape[2]
    core = lax.rem(my, 2)
    line = my // 2
    lines = m // 2
    partner = my + 1 - 2 * core

    def cols_of(i):
        return pl.ds(pl.multiple_of(i * wide, wide), wide)

    def line_peer(j):
        return lax.rem(line + j, lines) * 2 + core

    def line_source(j):
        return lax.rem(line + lines - j, lines) * 2 + core

    greet(
        [{"sp": lax.rem(me + k, n)} for k in range(1, n)]
        + [{"tp": partner}]
        + [{"tp": line_peer(j)} for j in range(1, lines)]
    )

    def cross(k):
        peer = across(me, k, n)
        return remote(x.at[peer], out.at[me, :, cols_of(my)], ss.at[k], sr.at[k], {"sp": peer})

    for k in range(1, n):
        cross(k).start()
    own = pltpu.make_async_copy(x.at[me], out.at[me, :, cols_of(my)], local)
    own.start()

    def block(s, i):
        return out.at[s, :, cols_of(i)]

    def to_line(k, s, j, i):
        return remote(block(s, i), block(s, i), ys.at[k, j], yr.at[k, j], {"tp": line_peer(j)})

    def to_core(k, s, i):
        return remote(block(s, i), block(s, i), cs.at[k], cr.at[k], {"tp": partner})

    def forward(k, s, j, i):
        return remote(block(s, i), block(s, i), fs.at[k, j], fr.at[k, j], {"tp": partner})

    def source(k):
        return across(me, k, n)

    def hand_on(k, s):
        for j in range(1, lines):
            to_line(k, s, j, my).start()
        to_core(k, s, my).start()

    def pass_on(k, s):
        for j in range(1, lines):
            i = line_source(j)
            to_line(k, s, j, i).wait_recv()
            forward(k, s, j, i).start()

    own.wait()
    hand_on(0, me)
    for k in range(1, n):
        s = source(k)
        remote(x.at[0], block(s, my), ss.at[k], sr.at[k], {"sp": s}).wait_recv()
        hand_on(k, s)
        pass_on(k - 1, source(k - 1))
    pass_on(n - 1, source(n - 1))
    for k in range(n):
        s = source(k)
        if k > 0:
            cross(k).wait_send()
        to_core(k, s, my).wait_send()
        to_core(k, s, partner).wait_recv()
        for j in range(1, lines):
            i = line_source(j)
            to_line(k, s, j, my).wait_send()
            forward(k, s, j, i).wait_send()
            forward(k, s, j, i + 1 - 2 * core).wait_recv()


def return_kernel(n, m, x, out, inbox, mid, midbox, last, cs, cr, ys, yr, ss, sr):
    me = lax.axis_index("sp")
    my = lax.axis_index("tp")
    wide = out.shape[2]
    core = lax.rem(my, 2)
    line = my // 2
    lines = m // 2
    partner = my + 1 - 2 * core

    def cols_of(i):
        return pl.ds(pl.multiple_of(i * wide, wide), wide)

    def line_at(j):
        return lax.rem(line + j, lines)

    greet(
        [{"sp": lax.rem(me + k, n)} for k in range(1, n)]
        + [{"tp": partner}]
        + [{"tp": line_at(j) * 2 + core} for j in range(1, lines)]
    )

    def place(k):
        return across(me, n - 1 - k, n)

    def to_core(k, j):
        i = line_at(j) * 2 + 1 - core
        return remote(x.at[place(k), :, cols_of(i)], inbox.at[k, j], cs.at[k, j], cr.at[k, j], {"tp": partner})

    def to_line(k, j):
        return remote(
            mid.at[k, j], midbox.at[k, j], ys.at[k, j], yr.at[k, j], {"tp": line_at(j) * 2 + core}
        )

    def cross(k):
        peer = place(k)
        return remote(last.at[k], out.at[me], ss.at[k], sr.at[k], {"sp": peer})

    for k in range(n):
        for j in reversed(range(lines)):
            to_core(k, j).start()

    def first(k):
        for j in reversed(range(lines)):
            to_core(k, j).wait_recv()
            i = line_at(j) * 2 + core
            mine = x[place(k), :, cols_of(i)].astype(F32) + inbox[k, j].astype(F32)
            mid[k, j] = mine.astype(BF16)
            if j > 0:
                to_line(k, j).start()

    def second(k):
        total = mid[k, 0].astype(F32)
        for j in range(1, lines):
            to_line(k, j).wait_recv()
            total = total + midbox[k, j].astype(F32)
        if k < n - 1:
            last[k] = total.astype(BF16)
            cross(k).start()
        else:
            out[me] = total.astype(BF16)

    first(0)
    for k in range(1, n):
        first(k)
        second(k - 1)
    second(n - 1)
    for k in range(n):
        for j in range(lines):
            to_core(k, j).wait_send()
            if j > 0:
                to_line(k, j).wait_send()
        if k < n - 1:
            cross(k).wait_send()
            s = place(k)
            remote(last.at[k], out.at[s], ss.at[k], sr.at[k], {"sp": s}).wait_recv()


def finish_kernel(n, capacity, experts, routes, affinity, pieces, settled, gain, out, term, mixture, send, recv):
    me = lax.axis_index("tp")
    rows = routes.shape[0]
    own = rows // n
    wide = pieces.shape[1]
    greet([{"tp": lax.rem(me + k, n)} for k in range(1, n)])

    def rows_of(i):
        return pl.ds(pl.multiple_of(i * own, own), own)

    def cols_of(i):
        return pl.ds(pl.multiple_of(i * wide, wide), wide)

    slots = slots_of(routes[...], capacity, experts)
    weights = affinity[...] / jnp.sum(affinity[...], axis=-1, keepdims=True)
    lane = lax.broadcasted_iota(jnp.int32, (rows, experts * capacity), 1)
    total = jnp.zeros((rows, wide), F32)
    for i, slot in enumerate(slots):
        hot = jnp.where(lane == slot, 1.0, 0.0).astype(BF16)
        total = total + weights[:, i : i + 1] * mm(hot, pieces[...])
    term[...] = total.astype(BF16)
    copies = []
    for k in range(1, n):
        peer = lax.rem(me + k, n)
        copy = remote(term.at[rows_of(peer), :], mixture.at[:, cols_of(me)], send.at[k], recv.at[k], {"tp": peer})
        copy.start()
        copies.append(copy)
    mixture[:, cols_of(me)] = term[rows_of(me), :]
    for k in range(1, n):
        source = lax.rem(me + n - k, n)
        copies[k - 1].wait_send()
        remote(
            term.at[rows_of(source), :], mixture.at[:, cols_of(source)], send.at[k], recv.at[k], {"tp": source}
        ).wait_recv()
    out[...] = layer_norm(settled[...] + mixture[...].astype(F32), gain[...]).astype(BF16)


def call(kernel, outs, scratch, count, collective_id=None):
    single = not isinstance(outs, list)
    return pl.pallas_call(
        kernel,
        out_shape=outs,
        in_specs=[VMEM] * count,
        out_specs=VMEM if single else [VMEM] * len(outs),
        scratch_shapes=scratch,
        compiler_params=params(collective_id),
    )


def body(
    query_one,
    key_one,
    value_one,
    gate_one,
    decay_one,
    query_two,
    key_two,
    value_two,
    gate_two,
    decay_two,
    head_gain,
    proj_one,
    proj_two,
    stream,
    gain_mix,
    gain_moe,
    routes,
    affinity,
    expert_gate,
    expert_up,
    expert_down,
):
    shape = jax.ShapeDtypeStruct
    rows = query_one.shape[0]
    n = lax.axis_size("sp")
    m = lax.axis_size("tp")
    width = stream.shape[1]
    own = rows // m
    wide = width // m
    dv = head_gain.shape[0]
    lanes = query_one.shape[1] + query_two.shape[1]
    values = value_one.shape[1] + value_two.shape[1]
    local_experts = expert_gate.shape[0]
    experts = local_experts * n
    top = routes.shape[1]
    capacity = 3 * rows * top // (2 * experts)
    room = local_experts * capacity

    half = dv // 2
    inputs = (key_one, value_one, decay_one, key_two, value_two, decay_two)
    stack, cum = pl.pallas_call(
        state_kernel,
        out_shape=[shape((2, 2, half + 16, lanes), BF16), shape((2, rows, lanes), F32)],
        in_specs=[pl.BlockSpec(memory_space=pltpu.HBM)] * len(inputs),
        out_specs=[VMEM] * 2,
        scratch_shapes=[pltpu.VMEM(a.shape, a.dtype) for a in inputs] + [DMA((len(inputs),))],
        compiler_params=pltpu.CompilerParams(vmem_limit_bytes=60 * 1024 * 1024),
    )(*inputs)
    chunks = max(1, lanes // 256)
    states = call(
        functools.partial(states_exchange_kernel, n),
        shape((2, 2, half, lanes), BF16),
        [
            pltpu.VMEM((2, half + 16, lanes), BF16),
            pltpu.VMEM((2, half + 16, lanes), BF16),
            pltpu.VMEM((n // 2, half + 16, lanes), BF16),
            pltpu.VMEM((2, half, lanes), BF16),
            DMA((chunks,)), DMA((chunks,)), DMA((chunks, n // 2)), DMA((chunks, n // 2)),
            DMA((chunks,)), DMA((chunks,)),
        ],
        1,
        1,
    )(stack)
    part = call(mix_kernel, shape((rows, width), BF16), [pltpu.VMEM((rows, values), BF16)], 13)(
        states, cum, query_one, key_one, value_one, gate_one, query_two, key_two, value_two, gate_two,
        head_gain.reshape(1, -1), proj_one, proj_two,
    )
    settled, columns = call(
        functools.partial(settle_kernel, m),
        [shape((own, width), F32), shape((rows, wide), BF16)],
        [pltpu.VMEM((m // 2, own, width), BF16)] * 3
        + [pltpu.VMEM((own, width), BF16)]
        + [DMA((m // 2,))] * 4
        + [DMA((m,))] * 2,
        3,
        2,
    )(part, stream, gain_mix.reshape(1, -1))
    outgoing = call(
        functools.partial(pick_kernel, capacity, experts), shape((experts * capacity, wide), BF16), [], 2
    )(routes, columns)
    lines = m // 2
    received = call(
        functools.partial(dispatch_kernel, n, m),
        shape((n, room, width), BF16),
        [DMA((n,)), DMA((n,)), DMA((n, lines)), DMA((n, lines)), DMA((n,)), DMA((n,)),
         DMA((n, lines)), DMA((n, lines)), DMA],
        1,
        3,
    )(outgoing.reshape(n, room, wide))
    x = received.reshape(n, local_experts, capacity, width)
    results = []
    for e in range(local_experts):
        xe = x[:, e].reshape(n * capacity, width)
        gate = mm(xe, expert_gate[e])
        upward = mm(xe, expert_up[e])
        act = (jax.nn.silu(gate) * upward).astype(BF16)
        results.append(mm(act, expert_down[e]).astype(BF16).reshape(n, capacity, width))
    partial_value = results[0] if local_experts == 1 else jnp.concatenate(results, axis=1)
    pieces = call(
        functools.partial(return_kernel, n, m),
        shape((n, room, wide), BF16),
        [pltpu.VMEM((n, lines, room, wide), BF16)] * 3
        + [pltpu.VMEM((n, room, wide), BF16)]
        + [DMA((n, lines))] * 4
        + [DMA((n,))] * 2,
        1,
        4,
    )(partial_value)
    return call(
        functools.partial(finish_kernel, m, capacity, experts),
        shape((own, width), BF16),
        [pltpu.VMEM((rows, wide), BF16), pltpu.VMEM((own, width), BF16), DMA((m,)), DMA((m,))],
        5,
        5,
    )(routes, affinity, pieces.reshape(experts * capacity, wide), settled, gain_moe.reshape(1, -1))


def solution(mesh):
    return jax.shard_map(
        body,
        mesh=mesh,
        in_specs=(
            P("sp", "tp"),
            P("sp", "tp"),
            P("sp", "tp"),
            P("sp", "tp"),
            P(None, "sp", "tp"),
            P("sp", "tp"),
            P("sp", "tp"),
            P("sp", "tp"),
            P("sp", "tp"),
            P(None, "sp", "tp"),
            P(),
            P("tp", None),
            P("tp", None),
            P("sp", None),
            P(),
            P(),
            P("sp", None),
            P("sp", None),
            P("sp", None, "tp"),
            P("sp", None, "tp"),
            P("sp", "tp", None),
        ),
        out_specs=P(("sp", "tp"), None),
        check_vma=False,
    )
```
